32 devices in a mesh: ep: 4 (over y, x), tp: 8 (over z, core).
Axes of the slice: x: 2, y: 2, z: 4, core: 2. Of those that a mesh axis runs over, the one named last changes fastest.
Arguments:
- tokens: bfloat16 [256, 2048], P('ep', 'tp'), may hold values from -64 to 64
- mixer_gain: float32 [2048], replicated, may hold values from 0.1 to 1.9
- expert_gain: float32 [2048], replicated, may hold values from 0.1 to 1.9
- query_weight: bfloat16 [2048, 1024], P(None, 'tp'), may hold values from -0.125 to 0.125
- key_weight: bfloat16 [2048, 1024], P(None, 'tp'), may hold values from -0.125 to 0.125
- value_weight: bfloat16 [2048, 4, 256], P(None, None, 'tp'), may hold values from -0.125 to 0.125
- outgate_weight: bfloat16 [2048, 4, 256], P(None, None, 'tp'), may hold values from -0.125 to 0.125
- ingate_weight: bfloat16 [2048, 4], replicated, may hold values from -0.125 to 0.125
- forget_weight: bfloat16 [2048, 4], replicated, may hold values from -0.125 to 0.125
- forget_bias: float32 [4], replicated, may hold values from -1 to 4
- mixout_weight: bfloat16 [1024, 2048], replicated, may hold values from -0.1875 to 0.1875
- memory_state: float32 [256, 4, 256, 256], P('ep', None, 'tp'), may hold values from -0.6 to 0.6
- norm_state: float32 [256, 4, 256], P('ep'), may hold values from -0.6 to 0.6
- max_state: float32 [256, 4], P('ep'), may hold values from -4 to 4
- expert_gate: bfloat16 [64, 2048, 256], P(('ep', 'tp')), may hold values from -0.125 to 0.125
- expert_up: bfloat16 [64, 2048, 256], P(('ep', 'tp')), may hold values from -0.125 to 0.125
- expert_down: bfloat16 [64, 256, 2048], P(('ep', 'tp')), may hold values from -0.1875 to 0.1875
- routes: int32 [256, 2], P('ep'), may hold values from 0 to 15, all different within a row; in each aligned block of 64 rows (0 to 63, 64 to 127, ...) at most 16 rows name the same one
- route_weights: float32 [256, 2], P('ep'), may hold values from 0.1 to 1
Outputs:
- mixed_out: bfloat16 [256, 2048], P('ep', 'tp')
- memory_next: float32 [256, 4, 256, 256], P('ep', None, 'tp')
- norm_next: float32 [256, 4, 256], P('ep')
- max_next: float32 [256, 4], P('ep')
The draws below stay inside these ranges and needn't reach their ends.
Inputs may be any that keep to these rules, and one draw needn't show every extreme that they name: `routes`: each row names 2 different experts; in the rows of one index of ep (aligned blocks of 64 rows) no expert is named by more than 16 rows, a bound that some block reaches.
All inputs are finite; a program needn't handle non-finite values.
Results may differ from the reference program's by a relative error of at most 0.0079.
Values may be sent and summed in bfloat16 or wider, within the bound.
A program may use at most 64 MiB of HBM per device.

```python
import math
import jax
import jax.numpy as jnp
import numpy as np
from jax import lax

D = 2048
HEADS = 4
HEAD_DIM = 256
FF = 1024
FF_SPLIT = 4
TOPK = 2
SEQS = 64
BATCH = 256
EXPERTS = 16
CAP = 16
N_EP = 4


def draw_tokens(key, part):
    key_base, key_rows = jax.random.split(key, 2)
    column_scale = jnp.exp(jnp.log(4.0) * (jnp.arange(D, dtype=jnp.float32) / D - 0.5))
    base_draw = jnp.clip(jax.random.normal(key_base, (BATCH, D), jnp.float32), -6.0, 6.0)
    row_scale = jnp.exp(jax.random.uniform(key_rows, (BATCH, 1), jnp.float32, jnp.log(0.5), jnp.log(5.0)))
    return (base_draw * column_scale * row_scale).astype(jnp.bfloat16)


def level_of(own_key, shape, cuts, least, high):
    level, own = 1.0, jax.random.fold_in(own_key, 6)
    for dim, blocks in cuts:
        draws = jnp.exp(jax.random.uniform(jax.random.fold_in(own, dim), (blocks,), jnp.float32, least / len(cuts), high / len(cuts)))
        level = level * jnp.repeat(draws, shape[dim] // blocks).reshape([-1 if axis == dim else 1 for axis in range(len(shape))])
    return level


def deal_out(key, own, number, rows, amount, top, limit, lean):
    order = jax.random.permutation(key, amount)
    crowded, common = portions_of(amount, rows * top, limit, lean, True), portions_of(amount, rows * top, limit, lean, False)
    places = jnp.arange(amount)

    def named(lengths, turn):
        used = int((lengths > 0).sum())
        fixed = max(1, used // 4)
        moved = fixed + (places - fixed + turn * (used - fixed)) % max(1, amount - fixed)
        return jnp.zeros((amount,), jnp.int32).at[order[jnp.where(places < fixed, places, moved)]].set(jnp.asarray(lengths, jnp.int32))

    lengths = jnp.where(number % 4 == 0, named(crowded, number // 4), named(common, number - number // 4 - 1))
    mixed = jax.random.permutation(jax.random.fold_in(own, 3), amount)
    giver, sink = mixed[0:amount // 2 * 2:2], mixed[1:amount // 2 * 2:2]
    slack = jnp.minimum(lengths[giver] - 1, limit - lengths[sink]) // 2
    slack = jnp.where((giver == order[0]) | (sink == order[0]) | (lengths[sink] == 0), 0, jnp.maximum(slack, 0))
    moved = jax.random.randint(jax.random.fold_in(own, 4), (amount // 2,), 0, 1 << 20) % (slack + 1)
    lengths = lengths.at[giver].add(-moved).at[sink].add(moved)
    items = jnp.searchsorted(jnp.cumsum(lengths), jnp.arange(rows * top), side="right").astype(jnp.int32)
    listing = items.reshape(top, rows).T
    listing = listing[jax.random.permutation(jax.random.fold_in(own, 1), rows)]
    turn = jax.random.randint(jax.random.fold_in(own, 2), (rows, 1), 0, top)
    return jnp.take_along_axis(listing, (jnp.arange(top)[None, :] + turn) % top, axis=1)


def portions_of(number_of, total, most, slope, full):
    loads = [(1 << 20) // math.isqrt(standing ** slope) + 1 for standing in range(1, number_of + 1)]
    largest = most if full else min(most, max(-(-total // number_of), total * loads[0] // sum(loads)))
    least = 1 if total - largest >= number_of - 1 else 0
    counts, spare = [largest] + [least] * (number_of - 1), total - largest - least * (number_of - 1)
    while spare > 0:
        movable = [i for i in range(1, number_of) if counts[i] < largest] or [i for i in range(1, number_of) if counts[i] < most]
        whole, remaining = sum([loads[i] for i in movable]), spare
        for i in movable:
            addition = min(most - counts[i], max(1, remaining * loads[i] // whole), spare)
            counts[i] = counts[i] + addition
            spare = spare - addition
    return np.array(counts)


def gaussian(rng, shape, scale, bound, cuts=(), held_as=jnp.bfloat16):
    loudness = level_of(rng, shape, cuts, -0.22, 0.18) if cuts else 1.0
    array = jax.random.normal(rng, shape, jnp.float32) * scale * loudness
    return jnp.minimum(jnp.maximum(array, -bound), bound).astype(held_as)


def setup_inputs(seed: int = 0) -> dict:
    seeds = jax.random.split(jax.random.key(seed), 20)
    tokens = draw_tokens(jax.random.fold_in(seeds[19], 71), 0)
    mixer_gain = jnp.clip(1.0 + 0.18 * jax.random.normal(seeds[1], (D,), jnp.float32), 0.1, 1.9)
    expert_gain = jnp.clip(1.0 + 0.18 * jax.random.normal(seeds[2], (D,), jnp.float32), 0.1, 1.9)
    query_weight = gaussian(seeds[3], (D, HEADS * HEAD_DIM), D ** -0.5, 0.125, ((1, 8),))
    key_weight = gaussian(seeds[4], (D, HEADS * HEAD_DIM), D ** -0.5, 0.125, ((1, 8),))
    value_weight = gaussian(seeds[5], (D, HEADS, HEAD_DIM), D ** -0.5, 0.125, ((2, 8),))
    outgate_weight = gaussian(seeds[6], (D, HEADS, HEAD_DIM), D ** -0.5, 0.125, ((2, 8),))
    ingate_weight = gaussian(seeds[7], (D, HEADS), D ** -0.5, 0.125)
    forget_weight = gaussian(seeds[8], (D, HEADS), D ** -0.5, 0.125)
    forget_bias = jnp.clip(jax.random.uniform(seeds[9], (HEADS,), jnp.float32, -1.0, 4.0), -1.0, 4.0)
    mixout_weight = gaussian(seeds[10], (HEADS * HEAD_DIM, D), (HEADS * HEAD_DIM) ** -0.5, 0.1875)
    memory_state = gaussian(seeds[11], (BATCH, HEADS, HEAD_DIM, HEAD_DIM), 0.1, 0.6, ((0, 4), (2, 8)), jnp.float32)
    norm_state = gaussian(seeds[12], (BATCH, HEADS, HEAD_DIM), 0.1, 0.6, ((0, 4),), jnp.float32)
    max_state = gaussian(seeds[13], (BATCH, HEADS), 1.0, 4.0, ((0, 4),), jnp.float32)
    expert_gate = gaussian(seeds[14], (EXPERTS * FF_SPLIT, D, FF // FF_SPLIT), D ** -0.5, 0.125, ((0, 32),))
    expert_up = gaussian(seeds[15], (EXPERTS * FF_SPLIT, D, FF // FF_SPLIT), D ** -0.5, 0.125, ((0, 32),))
    expert_down = gaussian(seeds[16], (EXPERTS * FF_SPLIT, FF // FF_SPLIT, D), FF ** -0.5, 0.1875, ((0, 32),))
    routes_keys = jax.random.split(jax.random.fold_in(seeds[17], 1), BATCH // SEQS)
    routes_turns = jax.random.permutation(jax.random.fold_in(seeds[17], 3), BATCH // SEQS)
    routes = jax.vmap(lambda own, number: deal_out(jax.random.fold_in(seeds[17], 2), own, number, SEQS, EXPERTS, TOPK, CAP, 2))(routes_keys, routes_turns).reshape((BATCH, TOPK))
    route_weights = jnp.clip(jnp.exp(math.log(1.0) - 2.3025851 * jax.random.uniform(seeds[18], (BATCH, TOPK), jnp.float32) ** level_of(seeds[18], (BATCH, TOPK), ((0, 4),), -0.2, 0.2)), 0.1, 1.0)
    return dict(tokens=tokens, mixer_gain=mixer_gain, expert_gain=expert_gain, query_weight=query_weight, key_weight=key_weight, value_weight=value_weight, outgate_weight=outgate_weight, ingate_weight=ingate_weight, forget_weight=forget_weight, forget_bias=forget_bias, mixout_weight=mixout_weight, memory_state=memory_state, norm_state=norm_state, max_state=max_state, expert_gate=expert_gate, expert_up=expert_up, expert_down=expert_down, routes=routes, route_weights=route_weights)


eps = 1e-06

def run_expert(packed):
    row_block, gate_blocks, up_blocks, down_blocks = packed
    block_count, width, block_units = gate_blocks.shape
    gate_mat = jnp.moveaxis(gate_blocks, 0, 1).reshape(width, block_count * block_units)
    up_mat = jnp.moveaxis(up_blocks, 0, 1).reshape(width, block_count * block_units)
    down_mat = down_blocks.reshape(block_count * block_units, down_blocks.shape[2])
    gate_part = jnp.dot(row_block, gate_mat, preferred_element_type=jnp.float32)
    up_part = jnp.dot(row_block, up_mat, preferred_element_type=jnp.float32)
    hidden = (jax.nn.silu(gate_part) * up_part).astype(jnp.bfloat16)
    return jnp.dot(hidden, down_mat, preferred_element_type=jnp.float32).astype(jnp.bfloat16)

def reference(tokens, mixer_gain, expert_gain, query_weight, key_weight, value_weight, outgate_weight, ingate_weight, forget_weight, forget_bias, mixout_weight, memory_state, norm_state, max_state, expert_gate, expert_up, expert_down, routes, route_weights):
    row_count = tokens.shape[0]
    token_float = tokens.astype(jnp.float32)
    inverse = lax.rsqrt(lax.optimization_barrier(jnp.mean(token_float * token_float, axis=1, keepdims=True)) + eps)
    scaled = (token_float * mixer_gain).astype(jnp.bfloat16)
    query_full = (inverse * jnp.dot(scaled, query_weight, preferred_element_type=jnp.float32)).reshape(row_count, HEADS, HEAD_DIM)
    key_full = (inverse * jnp.dot(scaled, key_weight, preferred_element_type=jnp.float32) * HEAD_DIM ** (-0.5)).reshape(row_count, HEADS, HEAD_DIM)
    values = (inverse * jnp.dot(scaled, value_weight.reshape(D, HEADS * HEAD_DIM), preferred_element_type=jnp.float32)).reshape(row_count, HEADS, HEAD_DIM)
    outgate = (inverse * jnp.dot(scaled, outgate_weight.reshape(D, HEADS * HEAD_DIM), preferred_element_type=jnp.float32)).reshape(row_count, HEADS, HEAD_DIM)
    ingate = inverse * jnp.dot(scaled, ingate_weight, preferred_element_type=jnp.float32)
    logforget = jax.nn.log_sigmoid(inverse * jnp.dot(scaled, forget_weight, preferred_element_type=jnp.float32) + forget_bias)
    max_next = jnp.maximum(logforget + max_state, ingate)
    decay_rate = jnp.exp(logforget + max_state - max_next)
    inflow = jnp.exp(ingate - max_next)
    memory_next = decay_rate[:, :, None, None] * memory_state + inflow[:, :, None, None] * values[:, :, :, None] * key_full[:, :, None, :]
    norm_next = decay_rate[:, :, None] * norm_state + inflow[:, :, None] * key_full
    numerator = jnp.einsum('bhvk,bhk->bhv', memory_next, query_full, precision=lax.Precision.HIGHEST)
    denominator = jnp.maximum(jnp.abs(lax.optimization_barrier(jnp.sum(norm_next * query_full, axis=2))), jnp.exp(-max_next))
    gated_heads = (jax.nn.sigmoid(outgate) * (numerator / denominator[:, :, None])).astype(jnp.bfloat16)
    middle = (token_float + jnp.dot(gated_heads.reshape(row_count, HEADS * HEAD_DIM), mixout_weight, preferred_element_type=jnp.float32)).astype(jnp.bfloat16)
    middle_float = middle.astype(jnp.float32)
    inverse_two = lax.rsqrt(lax.optimization_barrier(jnp.mean(middle_float * middle_float, axis=1, keepdims=True)) + eps)
    normed = (middle_float * inverse_two * expert_gain).astype(jnp.bfloat16)
    grouped = routes.reshape(N_EP, SEQS * TOPK)
    onehot = (grouped[:, :, None] == jnp.arange(EXPERTS, dtype=jnp.int32)[None, None, :]).astype(jnp.int32)
    slot_rank = lax.optimization_barrier(jnp.sum(onehot * (jnp.cumsum(onehot, axis=1) - 1), axis=2))
    row_index = (jnp.arange(N_EP, dtype=jnp.int32)[:, None] * CAP + slot_rank).reshape(-1).astype(jnp.int32)
    expert_index = grouped.reshape(-1).astype(jnp.int32)
    token_index = (jnp.arange(row_count * TOPK, dtype=jnp.int32) // TOPK).astype(jnp.int32)
    buffer = jnp.zeros((EXPERTS, N_EP * CAP, D), jnp.bfloat16).at[expert_index, row_index].set(normed[token_index])
    gate_blocks = expert_gate.reshape(EXPERTS, FF_SPLIT, D, FF // FF_SPLIT)
    up_blocks = expert_up.reshape(EXPERTS, FF_SPLIT, D, FF // FF_SPLIT)
    down_blocks = expert_down.reshape(EXPERTS, FF_SPLIT, FF // FF_SPLIT, D)
    results = lax.map(run_expert, (buffer, gate_blocks, up_blocks, down_blocks))
    picked = results[expert_index, row_index].astype(jnp.float32).reshape(row_count, TOPK, D)
    shares = route_weights / lax.optimization_barrier(jnp.sum(route_weights, axis=1, keepdims=True))
    mixed_out = (middle_float + lax.optimization_barrier(jnp.sum(shares[:, :, None] * picked, axis=1))).astype(jnp.bfloat16)
    return (mixed_out, memory_next, norm_next, max_next)
```

```python
import functools

import jax
import jax.numpy as jnp
from jax import lax
from jax.experimental import pallas as pl
from jax.experimental.pallas import tpu as pltpu
from jax.sharding import PartitionSpec as P

FF_SPLIT = 4
MESH = pl.DeviceIdType.MESH
VMEM = pltpu.VMEM
eps = 1e-06
F32 = jnp.float32
BF16 = jnp.bfloat16
GROUP = 8
TRANS = (((1,), (1,)), ((), ()))


def dot_t(left, right):
    return lax.dot_general(left, right, TRANS, preferred_element_type=F32)


def per_head(columns, head_count, each, width):
    head = lax.broadcasted_iota(jnp.int32, (columns.shape[0], width), 1) // each
    out = jnp.zeros((columns.shape[0], width), F32)
    for h in range(head_count):
        out = jnp.where(head == h, columns[:, h : h + 1], out)
    return out


def send(source, slot, send_sem, recv_sem, other):
    return pltpu.make_async_remote_copy(
        src_ref=source,
        dst_ref=slot,
        send_sem=send_sem,
        recv_sem=recv_sem,
        device_id={"tp": other},
        device_id_type=MESH,
    )


def spread(n, me, source, slots, sems):
    chips, chip, core = n // 2, me // 2, lax.rem(me, 2)
    for d in range(1, chips):
        other = lax.rem(chip + d, chips) * 2 + core
        send(source, slots.at[me], sems.at[0], sems.at[1 + d], other).start()
    send(source, slots.at[me], sems.at[0], sems.at[1], chip * 2 + 1 - core).start()


def relay(n, me, slots, sems):
    chips, chip, core = n // 2, me // 2, lax.rem(me, 2)
    partner = chip * 2 + 1 - core
    for d in range(1, chips):
        held = slots.at[lax.rem(chip + chips - d, chips) * 2 + core]
        send(held, held, sems.at[0], sems.at[1 + d], partner).wait_recv()
        send(held, held, sems.at[0], sems.at[1], partner).start()
    part = slots.at[pl.ds(0, chips)]
    send(part, part, sems.at[0], sems.at[1], partner).wait_recv()


def sent(n, slots, sems):
    part = slots.at[pl.ds(0, n - 1)]
    send(part, part, sems.at[0], sems.at[1], lax.axis_index("tp")).wait_send()


def bytes_wait(part, send_sem, recv_sem, here):
    done = pltpu.make_async_remote_copy(
        src_ref=part,
        dst_ref=part,
        send_sem=send_sem,
        recv_sem=recv_sem,
        device_id=here,
        device_id_type=MESH,
    )
    return done


def project_kernel(
    n,
    head_dim,
    tok,
    gain,
    wq_hbm,
    wk_hbm,
    wv_hbm,
    wo_hbm,
    wi,
    wf,
    bias,
    max_t,
    x_out,
    q_out,
    k_out,
    inflow_values,
    sig_out,
    decay_out,
    inflow_out,
    max_out,
    slots,
    qks,
    wq,
    wk,
    wv,
    wo,
    scaled,
    load_sems,
    sems,
    qk_sems,
):
    me = lax.axis_index("tp")
    loads = [
        pltpu.make_async_copy(a, b, load_sems.at[i])
        for i, (a, b) in enumerate(((wq_hbm, wq), (wk_hbm, wk), (wv_hbm, wv), (wo_hbm, wo)))
    ]
    for one in loads:
        one.start()
    barrier = pltpu.get_barrier_semaphore()
    for d in range(1, n):
        pl.semaphore_signal(
            barrier, inc=1, device_id={"tp": lax.rem(me + d, n)}, device_id_type=MESH
        )
    pl.semaphore_wait(barrier, n - 1)
    spread(n, me, tok, slots, sems)
    slots[me] = tok[...]
    seqs, own = tok.shape
    relay(n, me, slots, sems)
    total = jnp.zeros((seqs, 1), F32)
    for j in range(n):
        part = slots[j].astype(F32)
        x_out[:, j * own : (j + 1) * own] = slots[j]
        total = total + jnp.sum(part * part, axis=1, keepdims=True)
        scaled[:, j * own : (j + 1) * own] = (part * gain[:, j * own : (j + 1) * own]).astype(BF16)
    inverse = lax.rsqrt(total / (n * own) + eps)
    sent(n, slots, sems)
    loads[0].wait()
    loads[1].wait()
    width = wq.shape[1]
    row = scaled[...]
    query = inverse * jnp.dot(row, wq[...], preferred_element_type=F32)
    key = inverse * jnp.dot(row, wk[...], preferred_element_type=F32) * head_dim ** (-0.5)
    qks[me, 0] = query
    qks[me, 1] = key
    spread(n, me, qks.at[me], qks, qk_sems)
    loads[2].wait()
    loads[3].wait()
    values = inverse * dot_t(row, wv[...])
    sig_out[...] = jax.nn.sigmoid(inverse * dot_t(row, wo[...]))
    head_count = wi.shape[0]
    ingate = inverse * dot_t(row, wi[...])
    logforget = jax.nn.log_sigmoid(inverse * dot_t(row, wf[...]) + bias[...])
    eye = (
        lax.broadcasted_iota(jnp.int32, (seqs, seqs), 0)
        == lax.broadcasted_iota(jnp.int32, (seqs, seqs), 1)
    ).astype(F32)
    max_state = lax.dot_general(
        eye, max_t[...], TRANS, precision=lax.Precision.HIGHEST, preferred_element_type=F32
    )
    max_next = jnp.maximum(logforget + max_state, ingate)
    decay = jnp.exp(logforget + max_state - max_next)
    inflow = jnp.exp(ingate - max_next)
    max_out[...] = max_next
    each = wv.shape[0] // head_count
    inflow_values[...] = values * per_head(inflow, head_count, each, wv.shape[0])
    for h in range(head_count):
        decay_out[:, h * head_dim : (h + 1) * head_dim] = jnp.broadcast_to(
            decay[:, h : h + 1], (seqs, head_dim)
        )
        inflow_out[:, h * head_dim : (h + 1) * head_dim] = jnp.broadcast_to(
            inflow[:, h : h + 1], (seqs, head_dim)
        )
    relay(n, me, qks, qk_sems)
    for j in range(n):
        q_out[:, j * width : (j + 1) * width] = qks[j, 0]
        k_out[:, j * width : (j + 1) * width] = qks[j, 1]
    sent(n, qks, qk_sems)


def memory_kernel(
    q_ref,
    k_ref,
    inflow_values,
    sig,
    decay,
    inflow,
    max_ref,
    norm_ref,
    mem_hbm,
    mem_out,
    norm_out,
    gated,
    mem,
    denominators,
    in_sems,
    out_sems,
):
    seqs, head_count, each, head_dim = mem.shape
    groups = seqs // GROUP

    def chunk(g):
        return pl.ds(g * GROUP, GROUP)

    def load(g):
        return pltpu.make_async_copy(mem_hbm.at[chunk(g)], mem.at[chunk(g)], in_sems.at[g])

    def store(g):
        return pltpu.make_async_copy(mem.at[chunk(g)], mem_out.at[chunk(g)], out_sems.at[g])

    for g in range(groups):
        load(g).start()
    floor = jnp.exp(-max_ref[...])
    columns = []
    for h in range(head_count):
        span = slice(h * head_dim, (h + 1) * head_dim)
        fresh = decay[:, span] * norm_ref[:, h, :] + inflow[:, span] * k_ref[:, span]
        norm_out[:, h, :] = fresh
        mass = jnp.abs(jnp.sum(fresh * q_ref[:, span], axis=1, keepdims=True))
        columns.append(jnp.maximum(mass, floor[:, h : h + 1]))
    denominators[...] = per_head(
        jnp.concatenate(columns, axis=1), head_count, each, head_count * each
    )

    def body(g, _):
        load(g).wait()
        rows = pl.ds(pl.multiple_of(g * GROUP, GROUP), GROUP)
        lane = lax.broadcasted_iota(jnp.int32, (each, GROUP), 1)
        sides = jnp.transpose(inflow_values[rows, :])
        recalled = []
        for h in range(head_count):
            span = slice(h * head_dim, (h + 1) * head_dim)
            query, key, rate = q_ref[rows, span], k_ref[rows, span], decay[rows, span]
            found = jnp.zeros((each, GROUP), F32)
            for s in range(GROUP):
                side = sides[h * each : (h + 1) * each, s : s + 1]
                fresh = rate[s : s + 1] * mem[g * GROUP + s, h] + side * key[s : s + 1]
                mem[g * GROUP + s, h] = fresh
                total = jnp.sum(fresh * query[s : s + 1], axis=1, keepdims=True)
                found = jnp.where(lane == s, total, found)
            recalled.append(found)
        store(g).start()
        recall = jnp.transpose(jnp.concatenate(recalled, axis=0))
        gated[rows, :] = sig[rows, :] * (recall / denominators[rows, :])
        return 0

    lax.fori_loop(0, groups, body, 0)
    for g in range(groups):
        store(g).wait()


def experts_kernel(
    n_ep,
    n_tp,
    head_count,
    rows_each,
    local_experts,
    sharers,
    x_ref,
    gated,
    gain,
    mix_hbm,
    gate_hbm,
    up_hbm,
    down_hbm,
    routes_t,
    weights_t,
    out_ref,
    heads,
    own_heads,
    mix,
    gate,
    up,
    down,
    middle,
    outrows,
    inrows,
    parts,
    back,
    load_sems,
    sems,
    head_sems,
):
    ep, tp = lax.axis_index("ep"), lax.axis_index("tp")
    me = ep * n_tp + tp
    count = n_ep * n_tp
    seqs, width = x_ref.shape
    own = width // n_tp
    piece = gated.shape[1]
    peer = {"tp": lax.rem(tp + 1, n_tp)}
    blocks = gate_hbm.shape[0]
    each = piece // head_count
    head_dim = each * n_tp
    for h in range(head_count):
        for t in range(n_tp):
            pltpu.make_async_copy(
                mix_hbm.at[pl.ds(h * head_dim + t * each, each)],
                mix.at[pl.ds(t * piece + h * each, each)],
                load_sems.at[0],
            ).start()
    loads = [
        pltpu.make_async_copy(a, b, load_sems.at[i + 1])
        for i, (a, b) in enumerate(((gate_hbm, gate), (up_hbm, up), (down_hbm, down)))
    ]
    for one in loads:
        one.start()
    barrier = pltpu.get_barrier_semaphore()

    def greet(d, _):
        other = lax.rem(me + d, count)
        pl.semaphore_signal(
            barrier,
            inc=1,
            device_id={"ep": other // n_tp, "tp": lax.rem(other, n_tp)},
            device_id_type=MESH,
        )
        return 0

    lax.fori_loop(1, count, greet, 0)
    heads[tp] = gated[...].astype(BF16)
    pl.semaphore_wait(barrier, count - 1)
    spread(n_tp, tp, heads.at[tp], heads, head_sems)

    experts = local_experts * n_ep
    names = lax.broadcasted_iota(jnp.int32, (experts, seqs), 0)
    topk = routes_t.shape[0]
    chosen = [(routes_t[k : k + 1, :] == names).astype(F32) for k in range(topk)]
    earlier = (
        lax.broadcasted_iota(jnp.int32, (seqs, seqs), 0)
        < lax.broadcasted_iota(jnp.int32, (seqs, seqs), 1)
    ).astype(BF16)
    everyone = chosen[0]
    for k in range(1, topk):
        everyone = everyone + chosen[k]
    before = jnp.dot(everyone.astype(BF16), earlier, preferred_element_type=F32)
    targets = []
    for k in range(topk):
        slot = jnp.sum(chosen[k] * before, axis=0, keepdims=True).astype(jnp.int32)
        targets.append(routes_t[k : k + 1, :] * rows_each + slot)
        before = before + chosen[k]
    mine = tp // sharers
    place = lax.broadcasted_iota(jnp.int32, (n_ep * rows_each, seqs), 0)
    place = (place // rows_each * local_experts + mine) * rows_each + lax.rem(place, rows_each)
    picker = jnp.zeros(place.shape, F32)
    for k in range(topk):
        picker = picker + (place == targets[k]).astype(F32)
    picker = picker.astype(BF16)
    weight_sum = jnp.sum(weights_t[...], axis=0, keepdims=True)
    spot = lax.broadcasted_iota(jnp.int32, (count * rows_each, seqs), 0)
    source = spot // rows_each
    spot = (
        source // n_tp * local_experts + lax.rem(source, n_tp) // sharers
    ) * rows_each + lax.rem(spot, rows_each)
    combiner = jnp.zeros(spot.shape, F32)
    for k in range(topk):
        combiner = combiner + jnp.where(
            spot == targets[k], weights_t[k : k + 1, :] / weight_sum, 0.0
        )
    combiner = jnp.transpose(combiner)
    upper = combiner.astype(BF16)
    lower = (combiner - upper.astype(F32)).astype(BF16)

    relay(n_tp, tp, heads, head_sems)
    pltpu.make_async_copy(mix_hbm, mix, load_sems.at[0]).wait()
    for t in range(n_tp):
        own_heads[:, t * piece : (t + 1) * piece] = heads[t]
    flat = own_heads[...]
    total = jnp.zeros((seqs, 1), F32)
    for t in range(n_tp):
        span = slice(t * own, (t + 1) * own)
        fresh = x_ref[:, span].astype(F32) + jnp.dot(
            flat, mix[:, span], preferred_element_type=F32
        )
        fresh = fresh.astype(BF16)
        middle[:, span] = fresh
        fresh = fresh.astype(F32)
        total = total + jnp.sum(fresh * fresh, axis=1, keepdims=True)
    inverse = lax.rsqrt(total / width + eps)
    for t in range(n_tp):
        span = slice(t * own, (t + 1) * own)
        normed = (middle[:, span].astype(F32) * inverse * gain[:, span]).astype(BF16)
        picked = jnp.dot(picker, normed, preferred_element_type=F32).astype(BF16)
        outrows[:, :, span] = picked.reshape(n_ep, rows_each, own)
    for d in range(1, n_ep):
        other = lax.rem(ep + d, n_ep)
        pltpu.make_async_remote_copy(
            src_ref=outrows.at[other],
            dst_ref=inrows.at[ep],
            send_sem=sems.at[2],
            recv_sem=sems.at[3],
            device_id={"ep": other},
            device_id_type=MESH,
        ).start()
    inrows[ep] = outrows[ep]
    sent(n_tp, heads, head_sems)
    for one in loads:
        one.wait()
    there = {"ep": lax.rem(ep + 1, n_ep)}
    wait = bytes_wait(inrows.at[pl.ds(0, n_ep - 1)], sems.at[2], sems.at[3], there)
    wait.wait_recv()
    rows = inrows[...].reshape(n_ep * rows_each, width)
    hidden = []
    for b in range(blocks):
        gate_part = jnp.dot(rows, gate[b], preferred_element_type=F32)
        up_part = jnp.dot(rows, up[b], preferred_element_type=F32)
        hidden.append((jax.nn.silu(gate_part) * up_part).astype(BF16))

    def send_part(e, t):
        pltpu.make_async_remote_copy(
            src_ref=parts.at[t, e],
            dst_ref=back.at[me],
            send_sem=sems.at[4],
            recv_sem=sems.at[5],
            device_id={"ep": e, "tp": t},
            device_id_type=MESH,
        ).start()

    def finish(step, _):
        t = lax.rem(tp + 1 + step, n_tp)
        span = pl.ds(pl.multiple_of(t * own, own), own)
        result = jnp.dot(hidden[0], down[0, :, span], preferred_element_type=F32)
        for b in range(1, blocks):
            result = result + jnp.dot(hidden[b], down[b, :, span], preferred_element_type=F32)
        parts[t] = result.astype(BF16).reshape(n_ep, rows_each, own)
        for d in range(1, n_ep):
            send_part(lax.rem(ep + d, n_ep), t)

        @pl.when(step < n_tp - 1)
        def _():
            send_part(ep, t)

        return 0

    lax.fori_loop(0, n_tp, finish, 0)
    back[me] = parts[tp, ep]
    wait.wait_send()
    wait = bytes_wait(back.at[pl.ds(0, count - 1)], sems.at[4], sems.at[5], peer)
    wait.wait_recv()
    returned = back[...].reshape(count * rows_each, own)
    combined = jnp.dot(upper, returned, preferred_element_type=F32) + jnp.dot(
        lower, returned, preferred_element_type=F32
    )
    kept = middle[:, pl.ds(pl.multiple_of(tp * own, own), own)].astype(F32)
    out_ref[...] = (kept + combined).astype(BF16)
    wait.wait_send()


def local(
    n_ep,
    n_tp,
    tokens,
    mixer_gain,
    expert_gain,
    query_weight,
    key_weight,
    value_weight,
    outgate_weight,
    ingate_weight,
    forget_weight,
    forget_bias,
    mixout_weight,
    memory_state,
    norm_state,
    max_state,
    expert_gate,
    expert_up,
    expert_down,
    routes,
    route_weights,
):
    seqs, own = tokens.shape
    width = mixer_gain.shape[0]
    head_count = ingate_weight.shape[1]
    head_dim = norm_state.shape[2]
    each = value_weight.shape[2]
    piece = head_count * each
    channels = head_count * head_dim
    shape = jax.ShapeDtypeStruct
    vmem = pl.BlockSpec(memory_space=pltpu.VMEM)
    anywhere = pl.BlockSpec(memory_space=pl.ANY)
    values_t = jnp.transpose(value_weight, (1, 2, 0)).reshape(piece, width)
    outgate_t = jnp.transpose(outgate_weight, (1, 2, 0)).reshape(piece, width)
    cols = query_weight.shape[1]
    x_full, query, key, inflow_values, sig, decay, inflow, max_next = pl.pallas_call(
        functools.partial(project_kernel, n_tp, head_dim),
        out_shape=(
            shape((seqs, width), BF16),
            shape((seqs, channels), F32),
            shape((seqs, channels), F32),
            shape((seqs, piece), F32),
            shape((seqs, piece), F32),
            shape((seqs, channels), F32),
            shape((seqs, channels), F32),
            shape((seqs, head_count), F32),
        ),
        in_specs=[vmem, vmem, anywhere, anywhere, anywhere, anywhere, vmem, vmem, vmem, vmem],
        out_specs=(vmem,) * 8,
        scratch_shapes=[
            VMEM((n_tp, seqs, own), BF16),
            VMEM((n_tp, 2, seqs, cols), F32),
            VMEM((width, cols), BF16),
            VMEM((width, cols), BF16),
            VMEM((piece, width), BF16),
            VMEM((piece, width), BF16),
            VMEM((seqs, width), BF16),
            pltpu.SemaphoreType.DMA((4,)),
            pltpu.SemaphoreType.DMA((n_tp // 2 + 1,)),
            pltpu.SemaphoreType.DMA((n_tp // 2 + 1,)),
        ],
        compiler_params=pltpu.CompilerParams(
            collective_id=0, has_side_effects=True, vmem_limit_bytes=16 * 2**20
        ),
        name="project",
    )(
        tokens,
        mixer_gain.reshape(1, width),
        query_weight,
        key_weight,
        values_t,
        outgate_t,
        ingate_weight.T,
        forget_weight.T,
        forget_bias.reshape(1, head_count),
        max_state.T,
    )
    groups = seqs // GROUP
    memory_next, norm_next, gated = pl.pallas_call(
        memory_kernel,
        out_shape=(
            shape(memory_state.shape, F32),
            shape(norm_state.shape, F32),
            shape((seqs, piece), F32),
        ),
        in_specs=[vmem] * 8 + [anywhere],
        out_specs=(anywhere, vmem, vmem),
        scratch_shapes=[
            VMEM(memory_state.shape, F32),
            VMEM((seqs, piece), F32),
            pltpu.SemaphoreType.DMA((groups,)),
            pltpu.SemaphoreType.DMA((groups,)),
        ],
        compiler_params=pltpu.CompilerParams(vmem_limit_bytes=24 * 2**20),
        name="memory",
    )(query, key, inflow_values, sig, decay, inflow, max_next, norm_state, memory_state)

    block_count = expert_gate.shape[0]
    local_experts = block_count * n_tp // FF_SPLIT
    sharers = FF_SPLIT // block_count
    expert_count = local_experts * n_ep
    capacity = max(2, 2 * seqs * routes.shape[1] // expert_count)
    rows_each = -(-capacity // 16) * 16
    count = n_ep * n_tp
    mixed_out = pl.pallas_call(
        functools.partial(
            experts_kernel, n_ep, n_tp, head_count, rows_each, local_experts, sharers
        ),
        out_shape=shape((seqs, own), BF16),
        in_specs=[vmem, vmem, vmem, anywhere, anywhere, anywhere, anywhere, vmem, vmem],
        out_specs=vmem,
        scratch_shapes=[
            VMEM((n_tp, seqs, piece), BF16),
            VMEM((seqs, channels), BF16),
            VMEM(mixout_weight.shape, BF16),
            VMEM(expert_gate.shape, BF16),
            VMEM(expert_up.shape, BF16),
            VMEM(expert_down.shape, BF16),
            VMEM((seqs, width), BF16),
            VMEM((n_ep, rows_each, width), BF16),
            VMEM((n_ep, rows_each, width), BF16),
            VMEM((n_tp, n_ep, rows_each, own), BF16),
            VMEM((count, rows_each, own), BF16),
            pltpu.SemaphoreType.DMA((4,)),
            pltpu.SemaphoreType.DMA((6,)),
            pltpu.SemaphoreType.DMA((n_tp // 2 + 1,)),
        ],
        compiler_params=pltpu.CompilerParams(
            collective_id=1, has_side_effects=True, vmem_limit_bytes=40 * 2**20
        ),
        name="experts",
    )(
        x_full,
        gated,
        expert_gain.reshape(1, width),
        mixout_weight,
        expert_gate,
        expert_up,
        expert_down,
        routes.T,
        route_weights.T,
    )
    return (mixed_out, memory_next, norm_next, max_next)


def solution(mesh):
    in_specs = (
        P("ep", "tp"),
        P(),
        P(),
        P(None, "tp"),
        P(None, "tp"),
        P(None, None, "tp"),
        P(None, None, "tp"),
        P(),
        P(),
        P(),
        P(),
        P("ep", None, "tp", None),
        P("ep", None, None),
        P("ep", None),
        P(("ep", "tp"), None, None),
        P(("ep", "tp"), None, None),
        P(("ep", "tp"), None, None),
        P("ep", None),
        P("ep", None),
    )
    out_specs = (P("ep", "tp"), P("ep", None, "tp", None), P("ep", None, None), P("ep", None))
    step = functools.partial(local, mesh.shape["ep"], mesh.shape["tp"])
    return jax.shard_map(step, mesh=mesh, in_specs=in_specs, out_specs=out_specs, check_vma=False)
```

```python
import functools

import jax
import jax.numpy as jnp
from jax import lax
from jax.experimental import pallas as pl
from jax.experimental.pallas import tpu as pltpu
from jax.sharding import PartitionSpec as P

FF_SPLIT = 4
MESH = pl.DeviceIdType.MESH
VMEM = pltpu.VMEM
eps = 1e-06
F32 = jnp.float32
BF16 = jnp.bfloat16
GROUP = 8
TRANS = (((1,), (1,)), ((), ()))


def dot_t(left, right):
    return lax.dot_general(left, right, TRANS, preferred_element_type=F32)


def per_head(columns, head_count, each, width):
    head = lax.broadcasted_iota(jnp.int32, (columns.shape[0], width), 1) // each
    out = jnp.zeros((columns.shape[0], width), F32)
    for h in range(head_count):
        out = jnp.where(head == h, columns[:, h : h + 1], out)
    return out


def send(source, slot, send_sem, recv_sem, other):
    return pltpu.make_async_remote_copy(
        src_ref=source,
        dst_ref=slot,
        send_sem=send_sem,
        recv_sem=recv_sem,
        device_id={"tp": other},
        device_id_type=MESH,
    )


def spread(n, me, source, slots, sems):
    chips, chip, core = n // 2, me // 2, lax.rem(me, 2)
    for d in range(1, chips):
        other = lax.rem(chip + d, chips) * 2 + core
        send(source, slots.at[me], sems.at[0], sems.at[1 + d], other).start()
    send(source, slots.at[me], sems.at[0], sems.at[1], chip * 2 + 1 - core).start()


def relay(n, me, slots, sems):
    chips, chip, core = n // 2, me // 2, lax.rem(me, 2)
    partner = chip * 2 + 1 - core
    for d in range(1, chips):
        held = slots.at[lax.rem(chip + chips - d, chips) * 2 + core]
        send(held, held, sems.at[0], sems.at[1 + d], partner).wait_recv()
        send(held, held, sems.at[0], sems.at[1], partner).start()
    part = slots.at[pl.ds(0, chips)]
    send(part, part, sems.at[0], sems.at[1], partner).wait_recv()


def sent(n, slots, sems):
    part = slots.at[pl.ds(0, n - 1)]
    send(part, part, sems.at[0], sems.at[1], lax.axis_index("tp")).wait_send()


def bytes_wait(part, send_sem, recv_sem, here):
    done = pltpu.make_async_remote_copy(
        src_ref=part,
        dst_ref=part,
        send_sem=send_sem,
        recv_sem=recv_sem,
        device_id=here,
        device_id_type=MESH,
    )
    return done


def project_kernel(
    n,
    head_dim,
    tok,
    gain,
    wq_hbm,
    wk_hbm,
    wv_hbm,
    wo_hbm,
    wi,
    wf,
    bias,
    max_t,
    x_out,
    q_out,
    k_out,
    inflow_values,
    sig_out,
    decay_out,
    inflow_out,
    max_out,
    slots,
    qks,
    wq,
    wk,
    wv,
    wo,
    scaled,
    load_sems,
    sems,
    qk_sems,
):
    me = lax.axis_index("tp")
    loads = [
        pltpu.make_async_copy(a, b, load_sems.at[i])
        for i, (a, b) in enumerate(((wq_hbm, wq), (wk_hbm, wk), (wv_hbm, wv), (wo_hbm, wo)))
    ]
    for one in loads:
        one.start()
    barrier = pltpu.get_barrier_semaphore()
    for d in range(1, n):
        pl.semaphore_signal(
            barrier, inc=1, device_id={"tp": lax.rem(me + d, n)}, device_id_type=MESH
        )
    pl.semaphore_wait(barrier, n - 1)
    spread(n, me, tok, slots, sems)
    slots[me] = tok[...]
    seqs, own = tok.shape
    relay(n, me, slots, sems)
    total = jnp.zeros((seqs, 1), F32)
    for j in range(n):
        part = slots[j].astype(F32)
        x_out[:, j * own : (j + 1) * own] = slots[j]
        total = total + jnp.sum(part * part, axis=1, keepdims=True)
        scaled[:, j * own : (j + 1) * own] = (part * gain[:, j * own : (j + 1) * own]).astype(BF16)
    inverse = lax.rsqrt(total / (n * own) + eps)
    sent(n, slots, sems)
    loads[0].wait()
    loads[1].wait()
    width = wq.shape[1]
    row = scaled[...]
    query = inverse * jnp.dot(row, wq[...], preferred_element_type=F32)
    key = inverse * jnp.dot(row, wk[...], preferred_element_type=F32) * head_dim ** (-0.5)
    qks[me, 0] = query
    qks[me, 1] = key
    spread(n, me, qks.at[me], qks, qk_sems)
    loads[2].wait()
    loads[3].wait()
    values = inverse * dot_t(row, wv[...])
    sig_out[...] = jax.nn.sigmoid(inverse * dot_t(row, wo[...]))
    head_count = wi.shape[0]
    ingate = inverse * dot_t(row, wi[...])
    logforget = jax.nn.log_sigmoid(inverse * dot_t(row, wf[...]) + bias[...])
    eye = (
        lax.broadcasted_iota(jnp.int32, (seqs, seqs), 0)
        == lax.broadcasted_iota(jnp.int32, (seqs, seqs), 1)
    ).astype(F32)
    max_state = lax.dot_general(
        eye, max_t[...], TRANS, precision=lax.Precision.HIGHEST, preferred_element_type=F32
    )
    max_next = jnp.maximum(logforget + max_state, ingate)
    decay = jnp.exp(logforget + max_state - max_next)
    inflow = jnp.exp(ingate - max_next)
    max_out[...] = max_next
    each = wv.shape[0] // head_count
    inflow_values[...] = values * per_head(inflow, head_count, each, wv.shape[0])
    for h in range(head_count):
        decay_out[:, h * head_dim : (h + 1) * head_dim] = jnp.broadcast_to(
            decay[:, h : h + 1], (seqs, head_dim)
        )
        inflow_out[:, h * head_dim : (h + 1) * head_dim] = jnp.broadcast_to(
            inflow[:, h : h + 1], (seqs, head_dim)
        )
    relay(n, me, qks, qk_sems)
    for j in range(n):
        q_out[:, j * width : (j + 1) * width] = qks[j, 0]
        k_out[:, j * width : (j + 1) * width] = qks[j, 1]
    sent(n, qks, qk_sems)


def memory_kernel(
    q_ref,
    k_ref,
    inflow_values,
    sig,
    decay,
    inflow,
    max_ref,
    norm_ref,
    mem_hbm,
    mem_out,
    norm_out,
    gated,
    mem,
    held,
    denominators,
    in_sems,
    out_sems,
):
    seqs, head_count, each, head_dim = mem.shape
    groups = seqs // GROUP

    def chunk(g):
        return pl.ds(g * GROUP, GROUP)

    def load(g):
        return pltpu.make_async_copy(mem_hbm.at[chunk(g)], mem.at[chunk(g)], in_sems.at[g])

    def store(g):
        return pltpu.make_async_copy(held.at[chunk(g)], mem_out.at[chunk(g)], out_sems.at[g])

    for g in range(groups):
        load(g).start()
    floor = jnp.exp(-max_ref[...])
    columns = []
    for h in range(head_count):
        span = slice(h * head_dim, (h + 1) * head_dim)
        fresh = decay[:, span] * norm_ref[:, h, :] + inflow[:, span] * k_ref[:, span]
        norm_out[:, h, :] = fresh
        mass = jnp.abs(jnp.sum(fresh * q_ref[:, span], axis=1, keepdims=True))
        columns.append(jnp.maximum(mass, floor[:, h : h + 1]))
    denominators[...] = per_head(
        jnp.concatenate(columns, axis=1), head_count, each, head_count * each
    )

    def body(g, _):
        load(g).wait()
        rows = pl.ds(pl.multiple_of(g * GROUP, GROUP), GROUP)
        lane = lax.broadcasted_iota(jnp.int32, (each, GROUP), 1)
        sides = jnp.transpose(inflow_values[rows, :])
        recalled = []
        for h in range(head_count):
            span = slice(h * head_dim, (h + 1) * head_dim)
            query, key, rate = q_ref[rows, span], k_ref[rows, span], decay[rows, span]
            found = jnp.zeros((each, GROUP), F32)
            for s in range(GROUP):
                side = sides[h * each : (h + 1) * each, s : s + 1]
                fresh = rate[s : s + 1] * mem[g * GROUP + s, h] + side * key[s : s + 1]
                held[g * GROUP + s, h] = fresh
                total = jnp.sum(fresh * query[s : s + 1], axis=1, keepdims=True)
                found = jnp.where(lane == s, total, found)
            recalled.append(found)
        store(g).start()
        recall = jnp.transpose(jnp.concatenate(recalled, axis=0))
        gated[rows, :] = sig[rows, :] * (recall / denominators[rows, :])
        return 0

    lax.fori_loop(0, groups, body, 0)
    for g in range(groups):
        store(g).wait()


def experts_kernel(
    n_ep,
    n_tp,
    head_count,
    rows_each,
    local_experts,
    sharers,
    x_ref,
    gated,
    gain,
    mix_hbm,
    gate_hbm,
    up_hbm,
    down_hbm,
    routes_t,
    weights_t,
    out_ref,
    heads,
    own_heads,
    mix,
    gate,
    up,
    down,
    middle,
    outrows,
    inrows,
    parts,
    back,
    load_sems,
    sems,
    head_sems,
):
    ep, tp = lax.axis_index("ep"), lax.axis_index("tp")
    me = ep * n_tp + tp
    count = n_ep * n_tp
    seqs, width = x_ref.shape
    own = width // n_tp
    piece = gated.shape[1]
    peer = {"tp": lax.rem(tp + 1, n_tp)}
    blocks = gate_hbm.shape[0]
    each = piece // head_count
    head_dim = each * n_tp
    for h in range(head_count):
        for t in range(n_tp):
            pltpu.make_async_copy(
                mix_hbm.at[pl.ds(h * head_dim + t * each, each)],
                mix.at[pl.ds(t * piece + h * each, each)],
                load_sems.at[0],
            ).start()
    loads = [
        pltpu.make_async_copy(a, b, load_sems.at[i + 1])
        for i, (a, b) in enumerate(((gate_hbm, gate), (up_hbm, up), (down_hbm, down)))
    ]
    for one in loads:
        one.start()
    barrier = pltpu.get_barrier_semaphore()

    def greet(d, _):
        other = lax.rem(me + d, count)
        pl.semaphore_signal(
            barrier,
            inc=1,
            device_id={"ep": other // n_tp, "tp": lax.rem(other, n_tp)},
            device_id_type=MESH,
        )
        return 0

    lax.fori_loop(1, count, greet, 0)
    heads[tp] = gated[...].astype(BF16)
    pl.semaphore_wait(barrier, count - 1)
    spread(n_tp, tp, heads.at[tp], heads, head_sems)

    experts = local_experts * n_ep
    names = lax.broadcasted_iota(jnp.int32, (experts, seqs), 0)
    topk = routes_t.shape[0]
    chosen = [(routes_t[k : k + 1, :] == names).astype(F32) for k in range(topk)]
    earlier = (
        lax.broadcasted_iota(jnp.int32, (seqs, seqs), 0)
        < lax.broadcasted_iota(jnp.int32, (seqs, seqs), 1)
    ).astype(BF16)
    everyone = chosen[0]
    for k in range(1, topk):
        everyone = everyone + chosen[k]
    before = jnp.dot(everyone.astype(BF16), earlier, preferred_element_type=F32)
    targets = []
    for k in range(topk):
        slot = jnp.sum(chosen[k] * before, axis=0, keepdims=True).astype(jnp.int32)
        targets.append(routes_t[k : k + 1, :] * rows_each + slot)
        before = before + chosen[k]
    mine = tp // sharers
    place = lax.broadcasted_iota(jnp.int32, (n_ep * rows_each, seqs), 0)
    place = (place // rows_each * local_experts + mine) * rows_each + lax.rem(place, rows_each)
    picker = jnp.zeros(place.shape, F32)
    for k in range(topk):
        picker = picker + (place == targets[k]).astype(F32)
    picker = picker.astype(BF16)
    weight_sum = jnp.sum(weights_t[...], axis=0, keepdims=True)
    spot = lax.broadcasted_iota(jnp.int32, (count * rows_each, seqs), 0)
    source = spot // rows_each
    spot = (
        source // n_tp * local_experts + lax.rem(source, n_tp) // sharers
    ) * rows_each + lax.rem(spot, rows_each)
    combiner = jnp.zeros(spot.shape, F32)
    for k in range(topk):
        combiner = combiner + jnp.where(
            spot == targets[k], weights_t[k : k + 1, :] / weight_sum, 0.0
        )
    combiner = jnp.transpose(combiner)
    upper = combiner.astype(BF16)
    lower = (combiner - upper.astype(F32)).astype(BF16)

    relay(n_tp, tp, heads, head_sems)
    pltpu.make_async_copy(mix_hbm, mix, load_sems.at[0]).wait()
    for t in range(n_tp):
        own_heads[:, t * piece : (t + 1) * piece] = heads[t]
    flat = own_heads[...]
    total = jnp.zeros((seqs, 1), F32)
    for t in range(n_tp):
        span = slice(t * own, (t + 1) * own)
        fresh = x_ref[:, span].astype(F32) + jnp.dot(
            flat, mix[:, span], preferred_element_type=F32
        )
        fresh = fresh.astype(BF16)
        middle[:, span] = fresh
        fresh = fresh.astype(F32)
        total = total + jnp.sum(fresh * fresh, axis=1, keepdims=True)
    inverse = lax.rsqrt(total / width + eps)
    for t in range(n_tp):
        span = slice(t * own, (t + 1) * own)
        normed = (middle[:, span].astype(F32) * inverse * gain[:, span]).astype(BF16)
        picked = jnp.dot(picker, normed, preferred_element_type=F32).astype(BF16)
        outrows[:, :, span] = picked.reshape(n_ep, rows_each, own)
    for d in range(1, n_ep):
        other = lax.rem(ep + d, n_ep)
        pltpu.make_async_remote_copy(
            src_ref=outrows.at[other],
            dst_ref=inrows.at[ep],
            send_sem=sems.at[2],
            recv_sem=sems.at[3],
            device_id={"ep": other},
            device_id_type=MESH,
        ).start()
    inrows[ep] = outrows[ep]
    sent(n_tp, heads, head_sems)
    for one in loads:
        one.wait()
    there = {"ep": lax.rem(ep + 1, n_ep)}
    wait = bytes_wait(inrows.at[pl.ds(0, n_ep - 1)], sems.at[2], sems.at[3], there)
    wait.wait_recv()
    rows = inrows[...].reshape(n_ep * rows_each, width)
    hidden = []
    for b in range(blocks):
        gate_part = jnp.dot(rows, gate[b], preferred_element_type=F32)
        up_part = jnp.dot(rows, up[b], preferred_element_type=F32)
        hidden.append((jax.nn.silu(gate_part) * up_part).astype(BF16))

    def send_part(e, t):
        pltpu.make_async_remote_copy(
            src_ref=parts.at[t, e],
            dst_ref=back.at[me],
            send_sem=sems.at[4],
            recv_sem=sems.at[5],
            device_id={"ep": e, "tp": t},
            device_id_type=MESH,
        ).start()

    def finish(step, _):
        t = lax.rem(tp + 1 + step, n_tp)
        span = pl.ds(pl.multiple_of(t * own, own), own)
        result = jnp.dot(hidden[0], down[0, :, span], preferred_element_type=F32)
        for b in range(1, blocks):
            result = result + jnp.dot(hidden[b], down[b, :, span], preferred_element_type=F32)
        parts[t] = result.astype(BF16).reshape(n_ep, rows_each, own)
        for d in range(1, n_ep):
            send_part(lax.rem(ep + d, n_ep), t)

        @pl.when(step < n_tp - 1)
        def _():
            send_part(ep, t)

        return 0

    lax.fori_loop(0, n_tp, finish, 0)
    back[me] = parts[tp, ep]
    wait.wait_send()
    wait = bytes_wait(back.at[pl.ds(0, count - 1)], sems.at[4], sems.at[5], peer)
    wait.wait_recv()
    returned = back[...].reshape(count * rows_each, own)
    combined = jnp.dot(upper, returned, preferred_element_type=F32) + jnp.dot(
        lower, returned, preferred_element_type=F32
    )
    kept = middle[:, pl.ds(pl.multiple_of(tp * own, own), own)].astype(F32)
    out_ref[...] = (kept + combined).astype(BF16)
    wait.wait_send()


def local(
    n_ep,
    n_tp,
    tokens,
    mixer_gain,
    expert_gain,
    query_weight,
    key_weight,
    value_weight,
    outgate_weight,
    ingate_weight,
    forget_weight,
    forget_bias,
    mixout_weight,
    memory_state,
    norm_state,
    max_state,
    expert_gate,
    expert_up,
    expert_down,
    routes,
    route_weights,
):
    seqs, own = tokens.shape
    width = mixer_gain.shape[0]
    head_count = ingate_weight.shape[1]
    head_dim = norm_state.shape[2]
    each = value_weight.shape[2]
    piece = head_count * each
    channels = head_count * head_dim
    shape = jax.ShapeDtypeStruct
    vmem = pl.BlockSpec(memory_space=pltpu.VMEM)
    anywhere = pl.BlockSpec(memory_space=pl.ANY)
    values_t = jnp.transpose(value_weight, (1, 2, 0)).reshape(piece, width)
    outgate_t = jnp.transpose(outgate_weight, (1, 2, 0)).reshape(piece, width)
    cols = query_weight.shape[1]
    x_full, query, key, inflow_values, sig, decay, inflow, max_next = pl.pallas_call(
        functools.partial(project_kernel, n_tp, head_dim),
        out_shape=(
            shape((seqs, width), BF16),
            shape((seqs, channels), F32),
            shape((seqs, channels), F32),
            shape((seqs, piece), F32),
            shape((seqs, piece), F32),
            shape((seqs, channels), F32),
            shape((seqs, channels), F32),
            shape((seqs, head_count), F32),
        ),
        in_specs=[vmem, vmem, anywhere, anywhere, anywhere, anywhere, vmem, vmem, vmem, vmem],
        out_specs=(vmem,) * 8,
        scratch_shapes=[
            VMEM((n_tp, seqs, own), BF16),
            VMEM((n_tp, 2, seqs, cols), F32),
            VMEM((width, cols), BF16),
            VMEM((width, cols), BF16),
            VMEM((piece, width), BF16),
            VMEM((piece, width), BF16),
            VMEM((seqs, width), BF16),
            pltpu.SemaphoreType.DMA((4,)),
            pltpu.SemaphoreType.DMA((n_tp // 2 + 1,)),
            pltpu.SemaphoreType.DMA((n_tp // 2 + 1,)),
        ],
        compiler_params=pltpu.CompilerParams(
            collective_id=0, has_side_effects=True
        ),
        name="project",
    )(
        tokens,
        mixer_gain.reshape(1, width),
        query_weight,
        key_weight,
        values_t,
        outgate_t,
        ingate_weight.T,
        forget_weight.T,
        forget_bias.reshape(1, head_count),
        max_state.T,
    )
    groups = seqs // GROUP
    memory_next, norm_next, gated = pl.pallas_call(
        memory_kernel,
        out_shape=(
            shape(memory_state.shape, F32),
            shape(norm_state.shape, F32),
            shape((seqs, piece), F32),
        ),
        in_specs=[vmem] * 8 + [anywhere],
        out_specs=(anywhere, vmem, vmem),
        scratch_shapes=[
            VMEM(memory_state.shape, F32),
            VMEM(memory_state.shape, F32),
            VMEM((seqs, piece), F32),
            pltpu.SemaphoreType.DMA((groups,)),
            pltpu.SemaphoreType.DMA((groups,)),
        ],
        name="memory",
    )(query, key, inflow_values, sig, decay, inflow, max_next, norm_state, memory_state)

    block_count = expert_gate.shape[0]
    local_experts = block_count * n_tp // FF_SPLIT
    sharers = FF_SPLIT // block_count
    expert_count = local_experts * n_ep
    capacity = max(2, 2 * seqs * routes.shape[1] // expert_count)
    rows_each = -(-capacity // 16) * 16
    count = n_ep * n_tp
    mixed_out = pl.pallas_call(
        functools.partial(
            experts_kernel, n_ep, n_tp, head_count, rows_each, local_experts, sharers
        ),
        out_shape=shape((seqs, own), BF16),
        in_specs=[vmem, vmem, vmem, anywhere, anywhere, anywhere, anywhere, vmem, vmem],
        out_specs=vmem,
        scratch_shapes=[
            VMEM((n_tp, seqs, piece), BF16),
            VMEM((seqs, channels), BF16),
            VMEM(mixout_weight.shape, BF16),
            VMEM(expert_gate.shape, BF16),
            VMEM(expert_up.shape, BF16),
            VMEM(expert_down.shape, BF16),
            VMEM((seqs, width), BF16),
            VMEM((n_ep, rows_each, width), BF16),
            VMEM((n_ep, rows_each, width), BF16),
            VMEM((n_tp, n_ep, rows_each, own), BF16),
            VMEM((count, rows_each, own), BF16),
            pltpu.SemaphoreType.DMA((4,)),
            pltpu.SemaphoreType.DMA((6,)),
            pltpu.SemaphoreType.DMA((n_tp // 2 + 1,)),
        ],
        compiler_params=pltpu.CompilerParams(
            collective_id=1, has_side_effects=True
        ),
        name="experts",
    )(
        x_full,
        gated,
        expert_gain.reshape(1, width),
        mixout_weight,
        expert_gate,
        expert_up,
        expert_down,
        routes.T,
        route_weights.T,
    )
    return (mixed_out, memory_next, norm_next, max_next)


def solution(mesh):
    in_specs = (
        P("ep", "tp"),
        P(),
        P(),
        P(None, "tp"),
        P(None, "tp"),
        P(None, None, "tp"),
        P(None, None, "tp"),
        P(),
        P(),
        P(),
        P(),
        P("ep", None, "tp", None),
        P("ep", None, None),
        P("ep", None),
        P(("ep", "tp"), None, None),
        P(("ep", "tp"), None, None),
        P(("ep", "tp"), None, None),
        P("ep", None),
        P("ep", None),
    )
    out_specs = (P("ep", "tp"), P("ep", None, "tp", None), P("ep", None, None), P("ep", None))
    step = functools.partial(local, mesh.shape["ep"], mesh.shape["tp"])
    return jax.shard_map(step, mesh=mesh, in_specs=in_specs, out_specs=out_specs, check_vma=False)
```
